32 devices in a mesh: dp: 4 (over y, x), kv: 4 (over z), tp: 2 (over core).
Axes of the slice: x: 2, y: 2, z: 4, core: 2. Of those that a mesh axis runs over, the one named last changes fastest.
Arguments:
- tokens: bfloat16 [16, 4, 2048], P('dp', None, ('kv', 'tp')), may hold values from -6 to 6
- lengths: int32 [16], P('dp'), may hold values from 1 to 4, 24 in all
- carried: float32 [16, 16, 128, 128], P(('dp', 'kv'), 'tp'), may hold values from -4 to 4
- norm_mix: float32 [2048], replicated, may hold values from 0.1 to 1.9
- w_query: bfloat16 [2048, 16, 128], P(None, 'tp', 'kv'), may hold values from -0.125 to 0.125
- w_forget: bfloat16 [2048, 16, 128], P(None, 'tp', 'kv'), may hold values from -0.125 to 0.125
- w_input: bfloat16 [2048, 16, 128], P(None, 'tp', 'kv'), may hold values from -0.125 to 0.125
- w_gate: bfloat16 [2048, 16, 128], P(None, 'tp', 'kv'), may hold values from -0.125 to 0.125
- lower_bound: float32 [16, 128], P('tp'), may hold values from 0.3 to 0.9
- head_gain: float32 [128], replicated, may hold values from 0.1 to 1.9
- w_out: bfloat16 [16, 128, 2048], P('tp', None, 'kv'), may hold values from -0.125 to 0.125
- mixer_norm_gain: float32 [2048], replicated, may hold values from 0.1 to 1.9
- w_up: bfloat16 [2048, 8192], P(None, ('kv', 'tp')), may hold values from -0.125 to 0.125
- w_down: bfloat16 [8192, 2048], P(('kv', 'tp')), may hold values from -0.09375 to 0.09375
Outputs:
- result: bfloat16 [16, 4, 2048], P('dp', None, ('kv', 'tp'))
- new_state: float32 [16, 16, 128, 128], P(('dp', 'kv'), 'tp')
The draws below stay inside these ranges and needn't reach their ends.
Inputs may be any that keep to these rules, and one draw needn't show every extreme that they name: `lengths`: each sequence's number of live new token slots; some sequence has exactly 4.
All inputs are finite; a program needn't handle non-finite values. No bound on the sum of `lengths` on one device may be relied on, other than what follows from the above.
Results may differ from the reference program's by a relative error of at most 0.013.
Values may be sent and summed in bfloat16 or wider, within the bound.
A program may use at most 64 MiB of HBM per device.

```python
import math
import jax
import jax.numpy as jnp
import numpy as np
from jax import lax

D = 2048
HEADS = 16
HEAD_CHANNELS = 128
FF = 8192
NEW = 4
SEQS = 16


def strengthened(values, key, source, target, parts, factor):
    def block_of(axis_at):
        return (jnp.arange(values.shape[axis_at]) // (values.shape[axis_at] // parts)).reshape((-1,) + (1,) * (values.ndim - 1 - axis_at))

    first = jax.random.permutation(key, parts)[block_of(target)]
    far = (block_of(target) + parts // 2) % parts
    return jnp.where((block_of(source) == first) | (block_of(source) == far), factor * values, values)


def levels(key, shape, cuts, smallest, largest):
    level, own = 1.0, jax.random.fold_in(key, 6)
    for dim, parts in cuts:
        steps = jnp.exp(jax.random.uniform(jax.random.fold_in(own, dim), (parts,), jnp.float32, smallest / len(cuts), largest / len(cuts)))
        level = level * jnp.repeat(steps, shape[dim] // parts).reshape([-1 if axis == dim else 1 for axis in range(len(shape))])
    return level


def profile(amount, total, limit, lean):
    portions = [(1 << 20) // math.isqrt(grade ** lean) + 1 for grade in range(2, amount + 1)]
    spare, counts = total - limit - (amount - 1), [1] * (amount - 1)
    while spare > 0:
        free = [i for i in range(amount - 1) if counts[i] < limit]
        mass, remaining = sum([portions[i] for i in free]), spare
        for i in free:
            addition = min(limit - counts[i], max(1, remaining * portions[i] // mass), spare)
            counts[i] = counts[i] + addition
            spare = spare - addition
    return np.array([limit] + counts)


def ragged(rng, count, total, limit, skew):
    if count == 2:
        one = jax.random.randint(rng, (), max(1, total - limit), min(limit, total - 1) + 1)
        return jnp.stack([one, total - one])
    tallies = jnp.asarray(profile(count, total, limit, skew), jnp.int32)
    twos = (count - 1) // 2
    giver, taker = tallies[1:1 + 2 * twos:2], tallies[2:2 + 2 * twos:2]
    slack = jnp.minimum(giver - 1, limit - taker)
    passed = jax.random.randint(jax.random.fold_in(rng, 1), (twos,), 0, 1 << 20) % (slack + 1)
    tallies = tallies.at[1:1 + 2 * twos:2].set(giver - passed).at[2:2 + 2 * twos:2].set(taker + passed)
    return tallies[jax.random.permutation(jax.random.fold_in(rng, 2), count)]


def centred(own_key, extent, spread, reach, cuts=(), held_as=jnp.bfloat16):
    factor_of = levels(own_key, extent, cuts, -0.22, 0.18) if cuts else 1.0
    entries = jax.random.normal(own_key, extent, jnp.float32) * spread * factor_of
    return jnp.minimum(jnp.maximum(entries, -reach), reach).astype(held_as)


def noise_with(own_key, dims, spread, limit, shards, heavy, dtype=jnp.bfloat16):
    values = spread * jax.random.normal(own_key, dims, jnp.float32)
    if shards:
        values = values * levels(own_key, dims, shards, -0.22, 0.18)
    return jnp.clip(strengthened(values, jax.random.fold_in(own_key, 3), *heavy), -limit, limit).astype(dtype)


def setup_inputs(seed: int = 0) -> dict:
    arg_keys = jax.random.split(jax.random.key(seed), 15)
    tokens = centred(arg_keys[0], (SEQS, NEW, D), 1.0, 6.0, ((0, 4), (2, 8)))
    lengths = ragged(arg_keys[1], SEQS, SEQS + SEQS // 2, NEW, 2).astype(jnp.int32)
    carried = centred(arg_keys[2], (SEQS, HEADS, HEAD_CHANNELS, HEAD_CHANNELS), 0.5, 4.0, ((0, 16), (1, 2)), jnp.float32)
    norm_mix = jnp.clip(1.0 + 0.18 * jax.random.normal(arg_keys[3], (D,), jnp.float32), 0.1, 1.9)
    w_query = centred(arg_keys[4], (D, HEADS, HEAD_CHANNELS), D ** -0.5, 0.125, ((1, 2), (2, 4)))
    w_forget = centred(arg_keys[5], (D, HEADS, HEAD_CHANNELS), D ** -0.5, 0.125, ((1, 2), (2, 4)))
    w_input = centred(arg_keys[6], (D, HEADS, HEAD_CHANNELS), D ** -0.5, 0.125, ((1, 2), (2, 4)))
    w_gate = centred(arg_keys[7], (D, HEADS, HEAD_CHANNELS), D ** -0.5, 0.125, ((1, 2), (2, 4)))
    lower_bound = jnp.clip(0.3 + 0.59999996 * jax.random.uniform(arg_keys[8], (HEADS, HEAD_CHANNELS), jnp.float32) ** levels(arg_keys[8], (HEADS, HEAD_CHANNELS), ((0, 2),), -0.2, 0.2), 0.3, 0.9)
    head_gain = jnp.clip(1.0 + 0.18 * jax.random.normal(arg_keys[9], (HEAD_CHANNELS,), jnp.float32), 0.1, 1.9)
    w_out = centred(arg_keys[10], (HEADS, HEAD_CHANNELS, D), (HEADS * HEAD_CHANNELS) ** -0.5, 0.125, ((0, 2), (2, 4)))
    mixer_norm_gain = jnp.clip(1.0 + 0.18 * jax.random.normal(arg_keys[11], (D,), jnp.float32), 0.1, 1.9)
    w_up = centred(arg_keys[12], (D, FF), D ** -0.5, 0.125, ((1, 8),))
    w_down = noise_with(arg_keys[13], (FF, D), FF ** -0.5, 0.09375, ((0, 8),), (0, 1, 8, 2.0))
    return {"tokens": tokens, "lengths": lengths, "carried": carried, "norm_mix": norm_mix, "w_query": w_query, "w_forget": w_forget, "w_input": w_input, "w_gate": w_gate, "lower_bound": lower_bound, "head_gain": head_gain, "w_out": w_out, "mixer_norm_gain": mixer_norm_gain, "w_up": w_up, "w_down": w_down}


def norm_rows(values, gain):
    floated = values.astype(jnp.float32)
    scaled = floated * lax.rsqrt(lax.optimization_barrier(jnp.mean(floated * floated, axis=-1, keepdims=True)) + 1e-06)
    return (scaled * gain).astype(jnp.bfloat16)

def reference(tokens, lengths, carried, norm_mix, w_query, w_forget, w_input, w_gate, lower_bound, head_gain, w_out, mixer_norm_gain, w_up, w_down):
    normed = norm_rows(tokens, norm_mix).reshape(SEQS * NEW, D)

    def project(weight):
        flat = jnp.dot(normed, weight.reshape(D, HEADS * HEAD_CHANNELS), preferred_element_type=jnp.float32)
        return flat.astype(jnp.bfloat16).reshape(SEQS, NEW, HEADS, HEAD_CHANNELS)
    query_raw = project(w_query)
    forget_raw = project(w_forget)
    value_raw = project(w_input)
    gate_raw = project(w_gate)

    def per_sequence(inputs):
        query_in, forget_in, value_in, gate_in, length, outer_state = inputs
        query_vector = jax.nn.silu(query_in.astype(jnp.float32))
        forget = lower_bound + (1.0 - lower_bound) * jax.nn.sigmoid(forget_in.astype(jnp.float32))
        written = 1.0 - forget
        values = value_in.astype(jnp.float32)
        readouts = []
        for token_position in range(NEW):
            alive = token_position < length
            updated = forget[token_position][:, :, None] * outer_state + written[token_position][:, :, None] * values[token_position][:, None, :]
            outer_state = jnp.where(alive, updated, outer_state)
            state_readout = jnp.einsum('ts,tsz->tz', query_vector[token_position], outer_state, precision=lax.Precision.HIGHEST)
            readouts.append(jnp.where(alive, state_readout, jnp.float32(0.0)))
        state_readout = jnp.stack(readouts)
        scaled = state_readout * lax.rsqrt(lax.optimization_barrier(jnp.mean(state_readout * state_readout, axis=-1, keepdims=True)) + 1e-06)
        gated = scaled * head_gain * jax.nn.silu(gate_in.astype(jnp.float32))
        return (gated.astype(jnp.bfloat16), outer_state)
    mixed, new_state = lax.map(per_sequence, (query_raw, forget_raw, value_raw, gate_raw, lengths, carried))
    branch = jnp.dot(mixed.reshape(SEQS * NEW, HEADS * HEAD_CHANNELS), w_out.reshape(HEADS * HEAD_CHANNELS, D), preferred_element_type=jnp.float32)
    middle = (tokens.reshape(SEQS * NEW, D).astype(jnp.float32) + branch).astype(jnp.bfloat16)
    hidden_in = norm_rows(middle, mixer_norm_gain)
    upward = jnp.dot(hidden_in, w_up, preferred_element_type=jnp.float32)
    activated = jnp.square(jax.nn.relu(upward)).astype(jnp.bfloat16)
    down = jnp.dot(activated, w_down, preferred_element_type=jnp.float32)
    alive_rows = (jnp.arange(NEW)[None, :] < lengths[:, None]).reshape(SEQS * NEW, 1)
    result = jnp.where(alive_rows, middle.astype(jnp.float32) + down, jnp.float32(0.0)).astype(jnp.bfloat16)
    return (result.reshape(SEQS, NEW, D), new_state)
```

```python
import functools

import jax
import jax.numpy as jnp
from jax import lax
from jax.experimental import pallas as pl
from jax.experimental.pallas import tpu as pltpu
from jax.sharding import PartitionSpec as P


def norm_rows(values, gain):
    floated = values.astype(jnp.float32)
    scaled = floated * lax.rsqrt(jnp.mean(floated * floated, axis=-1, keepdims=True) + 1e-06)
    return (scaled * gain).astype(jnp.bfloat16)


def local_collectives(
    tokens,
    lengths,
    carried,
    norm_mix,
    w_query,
    w_forget,
    w_input,
    w_gate,
    lower_bound,
    head_gain,
    w_out,
    mixer_norm_gain,
    w_up,
    w_down,
):
    tp_size = lax.axis_size("tp")
    seq_group, new_rows, piece_width = tokens.shape
    seq_dev = carried.shape[0]
    gathered = lax.all_gather(tokens, ("kv", "tp"), axis=2, tiled=True)
    normed = norm_rows(gathered, norm_mix)
    model_width = gathered.shape[2]

    def project(weight):
        return jnp.einsum(
            "snd,dhk->snhk", normed, weight, preferred_element_type=jnp.float32
        ).astype(jnp.bfloat16)

    query_raw, forget_raw, value_raw, gate_raw = (
        lax.all_to_all(project(w_query), "kv", split_axis=0, concat_axis=3, tiled=True),
        lax.all_to_all(project(w_forget), "kv", split_axis=0, concat_axis=3, tiled=True),
        lax.all_to_all(project(w_input), "kv", split_axis=0, concat_axis=3, tiled=True),
        lax.all_to_all(project(w_gate), "kv", split_axis=0, concat_axis=3, tiled=True),
    )
    own_lengths = lax.dynamic_slice_in_dim(lengths, lax.axis_index("kv") * seq_dev, seq_dev)
    query_vector = jax.nn.silu(query_raw.astype(jnp.float32))
    forget = lower_bound + (1.0 - lower_bound) * jax.nn.sigmoid(forget_raw.astype(jnp.float32))
    written = 1.0 - forget
    values = value_raw.astype(jnp.float32)
    outer_state = carried
    readouts = []
    for token_position in range(new_rows):
        alive = (token_position < own_lengths)[:, None, None, None]
        updated = (
            forget[:, token_position, :, :, None] * outer_state
            + written[:, token_position, :, :, None] * values[:, token_position, :, None, :]
        )
        outer_state = jnp.where(alive, updated, outer_state)
        state_readout = jnp.einsum(
            "shk,shkv->shv",
            query_vector[:, token_position],
            outer_state,
            precision=lax.Precision.HIGHEST,
        )
        readouts.append(jnp.where(alive[..., 0], state_readout, jnp.float32(0.0)))
    state_readout = jnp.stack(readouts, axis=1)
    scaled = state_readout * lax.rsqrt(
        jnp.mean(state_readout * state_readout, axis=-1, keepdims=True) + 1e-06
    )
    mixed = (scaled * head_gain * jax.nn.silu(gate_raw.astype(jnp.float32))).astype(jnp.bfloat16)
    branch = jnp.einsum(
        "snhv,hvd->snd",
        lax.all_gather(mixed, "kv", axis=0, tiled=True),
        w_out,
        preferred_element_type=jnp.float32,
    )
    pair_width = piece_width * tp_size
    summed_total = lax.psum(branch, "tp")
    pair_cols = lax.dynamic_slice_in_dim(gathered, lax.axis_index("kv") * pair_width, pair_width, 2)
    pair_mid = (pair_cols.astype(jnp.float32) + summed_total).astype(jnp.bfloat16)
    full_pair = lax.all_gather(pair_mid, "kv", axis=2, tiled=True)
    middle = lax.dynamic_slice_in_dim(pair_mid, lax.axis_index("tp") * piece_width, piece_width, 2)
    hidden_in = norm_rows(full_pair, mixer_norm_gain).reshape(seq_group * new_rows, model_width)
    upward = jnp.dot(hidden_in, w_up, preferred_element_type=jnp.float32)
    activated = jnp.square(jax.nn.relu(upward)).astype(jnp.bfloat16)
    collected = lax.psum_scatter(
        jnp.einsum("fd,rf->dr", w_down, activated, preferred_element_type=jnp.float32),
        ("kv", "tp"),
        scatter_dimension=0,
        tiled=True,
    )
    down_part = collected.T.reshape(seq_group, new_rows, piece_width)
    alive_rows = (jnp.arange(new_rows)[None, :] < lengths[:, None])[:, :, None]
    result = jnp.where(alive_rows, middle.astype(jnp.float32) + down_part, jnp.float32(0.0)).astype(
        jnp.bfloat16
    )
    return (result, outer_state)


MESH = pl.DeviceIdType.MESH
F32 = jnp.float32
BF16 = jnp.bfloat16


def step_kernel(
    kv_size,
    tp_size,
    tokens,
    lengths,
    carried,
    norm_mix,
    w_query,
    w_forget,
    w_input,
    w_gate,
    lower_bound,
    head_gain,
    w_out,
    mixer_gain,
    w_up,
    w_down,
    result,
    new_state,
    tok_own,
    tok_all,
    wide,
    state_v,
    state_new,
    norm_v,
    w_proj,
    lower_v,
    head_v,
    w_out_v,
    mixer_v,
    w_up_v,
    w_down_v,
    raw_split,
    swap_src,
    swap_dst,
    by_slot,
    mix_src,
    mix_dst,
    mix_wide,
    pair_src,
    pair_dst,
    mid_src,
    mid_dst,
    red_src,
    red_dst,
    result_v,
    load_sem,
    send_tok,
    recv_tok,
    send_swap,
    recv_swap,
    send_mix,
    recv_mix,
    send_pair,
    recv_pair,
    send_mid,
    recv_mid,
    send_red,
    recv_red,
    store_sem,
):
    seqs, slots, piece = tok_own.shape
    group = kv_size * tp_size
    rows = seqs * slots
    heads, chans = lower_v.shape
    width = group * piece
    pair = tp_size * piece
    own_cols = w_proj.shape[1]
    sub = own_cols // heads
    per_tile = chans // sub
    kv = lax.axis_index("kv")
    tp = lax.axis_index("tp")
    me = kv * tp_size + tp

    loads = [
        pltpu.make_async_copy(tokens, tok_own, load_sem.at[0]),
        pltpu.make_async_copy(norm_mix, norm_v, load_sem.at[1]),
        pltpu.make_async_copy(w_query, w_proj.at[0], load_sem.at[2]),
        pltpu.make_async_copy(w_forget, w_proj.at[1], load_sem.at[3]),
        pltpu.make_async_copy(w_input, w_proj.at[2], load_sem.at[4]),
        pltpu.make_async_copy(w_gate, w_proj.at[3], load_sem.at[5]),
        pltpu.make_async_copy(lower_bound, lower_v, load_sem.at[6]),
        pltpu.make_async_copy(head_gain, head_v, load_sem.at[7]),
        pltpu.make_async_copy(carried, state_v, load_sem.at[8]),
        pltpu.make_async_copy(w_out, w_out_v, load_sem.at[9]),
        pltpu.make_async_copy(mixer_gain, mixer_v, load_sem.at[10]),
        pltpu.make_async_copy(w_up, w_up_v, load_sem.at[11]),
        pltpu.make_async_copy(w_down, w_down_v, load_sem.at[12]),
    ]
    for load in loads:
        load.start()

    def peer(step):
        other = lax.rem(me + step, group)
        return other, {"kv": other // tp_size, "tp": lax.rem(other, tp_size)}

    def column_peer(step):
        other = lax.rem(kv + step, kv_size)
        return other, {"kv": other, "tp": tp}

    barrier = pltpu.get_barrier_semaphore()
    for step in range(1, group):
        pl.semaphore_signal(barrier, inc=1, device_id=peer(step)[1], device_id_type=MESH)
    pl.semaphore_wait(barrier, group - 1)

    sent = []

    def send(src, dst, send_sem, recv_sem, device):
        copy = pltpu.make_async_remote_copy(
            src_ref=src,
            dst_ref=dst,
            send_sem=send_sem,
            recv_sem=recv_sem,
            device_id=device,
            device_id_type=MESH,
        )
        copy.start()
        sent.append(copy)

    def arrived(src, dst, send_sem, recv_sem, device):
        pltpu.make_async_remote_copy(
            src_ref=src,
            dst_ref=dst,
            send_sem=send_sem,
            recv_sem=recv_sem,
            device_id=device,
            device_id_type=MESH,
        ).wait_recv()

    def far_first(count):
        return sorted(range(1, count), key=lambda step: -min(step, count - step))

    loads[0].wait()
    for step in far_first(group):
        _, device = peer(step)
        send(tok_own, tok_all.at[me], send_tok.at[step], recv_tok.at[me], device)
    tok_all[pl.ds(me, 1)] = tok_own[...][None]
    for index in (1, 6, 7, 8):
        loads[index].wait()
    state_half = state_v[...].reshape(heads * chans, chans).astype(BF16)
    for step in range(1, group):
        other, device = peer(step)
        arrived(tok_own, tok_all.at[other], send_tok.at[step], recv_tok.at[other], device)
    for part in range(group):
        block = tok_all[part].astype(F32)
        for seq in range(seqs):
            wide[seq * slots : (seq + 1) * slots, part * piece : (part + 1) * piece] = block[seq]
    floated = wide[...]
    normed = (
        floated
        * lax.rsqrt(jnp.mean(floated * floated, axis=-1, keepdims=True) + 1e-06)
        * norm_v[...]
    ).astype(BF16)
    for matrix in range(4):
        loads[2 + matrix].wait()
        raw = lax.dot_general(
            normed, w_proj[matrix], (((1,), (1,)), ((), ())), preferred_element_type=F32
        )
        for seq in range(seqs):
            raw_split[seq, matrix * slots : (matrix + 1) * slots, :] = raw[
                seq * slots : (seq + 1) * slots
            ]
    swap_src[...] = raw_split[...].astype(BF16)
    for step in far_first(kv_size):
        other, device = column_peer(step)
        send(swap_src.at[other], swap_dst.at[kv], send_swap.at[step], recv_swap.at[kv], device)
    swap_dst[pl.ds(kv, 1)] = swap_src[pl.ds(kv, 1)]
    for step in range(1, kv_size):
        other, device = column_peer(step)
        arrived(
            swap_src.at[other],
            swap_dst.at[other],
            send_swap.at[step],
            recv_swap.at[other],
            device,
        )

    lane = lax.broadcasted_iota(jnp.int32, (4 * slots, chans), 1) // sub
    arrivals = [swap_dst[part].astype(F32) for part in range(kv_size)]
    for head in range(heads):
        tile, place = divmod(head, per_tile)
        joined = None
        for part in range(kv_size):
            piece_of = arrivals[part][:, tile * chans : (tile + 1) * chans]
            shift = ((part - place) * sub) % chans
            turned = pltpu.roll(piece_of, shift, 1) if shift else piece_of
            joined = turned if joined is None else jnp.where(lane == part, turned, joined)
        by_slot[:, head, :] = joined

    length = lengths[kv]
    lower = lower_v[...]
    queries, forgets, writes, values, gates = [], [], [], [], []
    for slot in range(slots):
        alive = slot < length
        query_raw = by_slot[slot]
        gate_raw = by_slot[3 * slots + slot]
        queries.append(query_raw * jax.nn.sigmoid(query_raw))
        gates.append(gate_raw * jax.nn.sigmoid(gate_raw))
        forget = lower + (1.0 - lower) * jax.nn.sigmoid(by_slot[slots + slot])
        forgets.append(jnp.where(alive, forget, 1.0))
        writes.append(jnp.where(alive, 1.0 - forget, 0.0))
        values.append(by_slot[2 * slots + slot])
    decayed, total = [], None
    for slot in range(slots):
        total = forgets[slot] if total is None else total * forgets[slot]
        decayed.append(queries[slot] * total)
    stacked = jnp.concatenate(decayed, axis=0)
    row_head = lax.broadcasted_iota(jnp.int32, (slots * heads, chans), 0) % heads
    spread = jnp.concatenate(
        [jnp.where(row_head == head, stacked, 0.0).astype(BF16) for head in range(heads)], axis=1
    )
    from_state = jnp.dot(spread, state_half, preferred_element_type=F32)
    kept = list(writes)
    for slot in range(slots):
        for earlier in range(slot):
            kept[earlier] = kept[earlier] * forgets[slot]
        readout = from_state[slot * heads : (slot + 1) * heads]
        for earlier in range(slot + 1):
            weight = jnp.sum(queries[slot] * kept[earlier], axis=-1, keepdims=True)
            readout = readout + weight * values[earlier]
        readout = jnp.where(slot < length, readout, 0.0)
        scaled = readout * lax.rsqrt(jnp.mean(readout * readout, axis=-1, keepdims=True) + 1e-06)
        mix_src[slot] = (scaled * head_v[...] * gates[slot]).astype(BF16)
    for step in far_first(kv_size):
        other, device = column_peer(step)
        send(mix_src, mix_dst.at[kv], send_mix.at[step], recv_mix.at[kv], device)
    mix_dst[pl.ds(kv, 1)] = mix_src[...][None]

    columns = jnp.concatenate([total] + kept, axis=0).T
    for head in range(heads):
        fresh = columns[:, head : head + 1] * state_v[head]
        for slot in range(slots):
            at = (slot + 1) * heads + head
            fresh = fresh + columns[:, at : at + 1] * values[slot][head : head + 1]
        state_new[head] = fresh
    state_store = pltpu.make_async_copy(state_new, new_state, store_sem.at[0])
    state_store.start()

    for step in range(1, kv_size):
        other, device = column_peer(step)
        arrived(mix_src, mix_dst.at[other], send_mix.at[step], recv_mix.at[other], device)
    mix_wide[...] = mix_dst[...].astype(F32).reshape(rows, heads, chans)
    mixed = jnp.concatenate([mix_wide[:, head, :].astype(BF16) for head in range(heads)], axis=1)
    loads[9].wait()
    partial = jnp.dot(mixed, w_out_v[...], preferred_element_type=F32)
    pair_src[...] = partial
    partner = {"kv": kv, "tp": lax.rem(tp + 1, tp_size)}
    send(pair_src, pair_dst, send_pair.at[0], recv_pair.at[0], partner)
    own_wide = wide[:, pl.ds(pl.multiple_of(kv * pair, pair), pair)]
    arrived(pair_src, pair_dst, send_pair.at[0], recv_pair.at[0], partner)
    mid_src[...] = (own_wide + (partial + pair_dst[...])).astype(BF16)
    for step in far_first(kv_size):
        other, device = column_peer(step)
        send(mid_src, mid_dst.at[kv], send_mid.at[step], recv_mid.at[kv], device)
    mid_dst[pl.ds(kv, 1)] = mid_src[...][None]
    for step in range(1, kv_size):
        other, device = column_peer(step)
        arrived(mid_src, mid_dst.at[other], send_mid.at[step], recv_mid.at[other], device)

    middle = jnp.concatenate([mid_dst[part].astype(F32) for part in range(kv_size)], axis=1)
    loads[10].wait()
    hidden = (
        middle
        * lax.rsqrt(jnp.mean(middle * middle, axis=-1, keepdims=True) + 1e-06)
        * mixer_v[...]
    ).astype(BF16)
    loads[11].wait()
    upward = jnp.dot(hidden, w_up_v[...], preferred_element_type=F32)
    activated = jnp.square(jnp.maximum(upward, 0.0)).astype(BF16)
    loads[12].wait()

    def down_piece(other):
        cols = pl.ds(pl.multiple_of(other * piece, piece), piece)
        return jnp.dot(activated, w_down_v[:, cols], preferred_element_type=F32)

    for step in far_first(group):
        other, device = peer(step)
        red_src[step] = down_piece(other).astype(BF16)
        send(red_src.at[step], red_dst.at[me], send_red.at[step], recv_red.at[me], device)
    down = down_piece(me)
    own_mid = mid_src[:, pl.ds(pl.multiple_of(tp * piece, piece), piece)].astype(F32)
    for step in range(1, group):
        other, device = peer(step)
        arrived(red_src.at[step], red_dst.at[other], send_red.at[step], recv_red.at[other], device)
        down = down + red_dst[other].astype(F32)
    done = own_mid + down
    slot_of = lax.broadcasted_iota(jnp.int32, (slots, piece), 0)
    for seq in range(seqs):
        kept_rows = jnp.where(
            slot_of < lengths[seq], done[seq * slots : (seq + 1) * slots], 0.0
        )
        result_v[seq] = kept_rows.astype(BF16)
    result_store = pltpu.make_async_copy(result_v, result, store_sem.at[1])
    result_store.start()
    for copy in sent:
        copy.wait_send()
    state_store.wait()
    result_store.wait()


def local_kernel(
    tokens,
    lengths,
    carried,
    norm_mix,
    w_query,
    w_forget,
    w_input,
    w_gate,
    lower_bound,
    head_gain,
    w_out,
    mixer_norm_gain,
    w_up,
    w_down,
):
    kv_size = lax.axis_size("kv")
    tp_size = lax.axis_size("tp")
    group = kv_size * tp_size
    seqs, slots, piece = tokens.shape
    _, heads, chans, _ = carried.shape
    model, _, sub = w_query.shape
    rows, pair, cols = seqs * slots, piece * tp_size, heads * sub
    hidden = w_up.shape[1]

    def turned(weight):
        return weight.transpose(1, 2, 0).reshape(cols, model)

    anywhere = pl.BlockSpec(memory_space=pl.ANY)
    dma = pltpu.SemaphoreType.DMA
    vmem = pltpu.VMEM
    result, new_state = pl.pallas_call(
        functools.partial(step_kernel, kv_size, tp_size),
        out_shape=(
            jax.ShapeDtypeStruct(tokens.shape, BF16),
            jax.ShapeDtypeStruct((heads, chans, chans), F32),
        ),
        in_specs=[anywhere, pl.BlockSpec(memory_space=pltpu.SMEM)] + [anywhere] * 12,
        out_specs=(anywhere, anywhere),
        scratch_shapes=[
            vmem((seqs, slots, piece), BF16),
            vmem((group, seqs, slots, piece), BF16),
            vmem((rows, model), F32),
            vmem((heads, chans, chans), F32),
            vmem((heads, chans, chans), F32),
            vmem((1, model), F32),
            vmem((4, cols, model), BF16),
            vmem((heads, chans), F32),
            vmem((1, chans), F32),
            vmem((heads * chans, pair), BF16),
            vmem((1, model), F32),
            vmem((model, hidden), BF16),
            vmem((hidden, model), BF16),
            vmem((seqs, 4 * slots, cols), F32),
            vmem((seqs, 4 * slots, cols), BF16),
            vmem((kv_size, 4 * slots, cols), BF16),
            vmem((4 * slots, heads, chans), F32),
            vmem((slots, heads, chans), BF16),
            vmem((kv_size, slots, heads, chans), BF16),
            vmem((rows, heads, chans), F32),
            vmem((rows, pair), F32),
            vmem((rows, pair), F32),
            vmem((rows, pair), BF16),
            vmem((kv_size, rows, pair), BF16),
            vmem((group, rows, piece), BF16),
            vmem((group, rows, piece), BF16),
            vmem((seqs, slots, piece), BF16),
            dma((13,)),
            dma((group,)),
            dma((group,)),
            dma((kv_size,)),
            dma((kv_size,)),
            dma((kv_size,)),
            dma((kv_size,)),
            dma((1,)),
            dma((1,)),
            dma((kv_size,)),
            dma((kv_size,)),
            dma((group,)),
            dma((group,)),
            dma((2,)),
        ],
        compiler_params=pltpu.CompilerParams(
            collective_id=0, has_side_effects=True, vmem_limit_bytes=60000 * 1024
        ),
    )(
        tokens,
        lengths,
        carried.reshape(heads, chans, chans),
        norm_mix.reshape(1, model),
        turned(w_query),
        turned(w_forget),
        turned(w_input),
        turned(w_gate),
        lower_bound,
        head_gain.reshape(1, chans),
        w_out.reshape(heads * chans, pair),
        mixer_norm_gain.reshape(1, model),
        w_up,
        w_down,
    )
    return result, new_state.reshape(carried.shape)


def local(*arrays):
    tokens, carried, weight = arrays[0], arrays[2], arrays[4]
    aligned = (
        tokens.shape[2] % 128 == 0
        and carried.shape[0] == 1
        and carried.shape[2] % 128 == 0
        and carried.shape[2] % weight.shape[2] == 0
        and (weight.shape[1] * weight.shape[2]) % carried.shape[2] == 0
        and lax.axis_size("tp") == 2
        and tokens.shape[1] % 4 == 0
    )
    return (local_kernel if aligned else local_collectives)(*arrays)


def solution(mesh):
    placed = (
        P("dp", None, ("kv", "tp")),
        P("dp"),
        P(("dp", "kv"), "tp", None, None),
        P(),
        P(None, "tp", "kv"),
        P(None, "tp", "kv"),
        P(None, "tp", "kv"),
        P(None, "tp", "kv"),
        P("tp", None),
        P(),
        P("tp", None, "kv"),
        P(),
        P(None, ("kv", "tp")),
        P(("kv", "tp"), None),
    )
    return jax.shard_map(
        local,
        mesh=mesh,
        in_specs=placed,
        out_specs=(P("dp", None, ("kv", "tp")), P(("dp", "kv"), "tp", None, None)),
        check_vma=False,
    )
```

```python
import functools

import jax
import jax.numpy as jnp
from jax import lax
from jax.experimental import pallas as pl
from jax.experimental.pallas import tpu as pltpu
from jax.sharding import PartitionSpec as P


def norm_rows(values, gain):
    floated = values.astype(jnp.float32)
    scaled = floated * lax.rsqrt(jnp.mean(floated * floated, axis=-1, keepdims=True) + 1e-06)
    return (scaled * gain).astype(jnp.bfloat16)


def local_collectives(
    tokens,
    lengths,
    carried,
    norm_mix,
    w_query,
    w_forget,
    w_input,
    w_gate,
    lower_bound,
    head_gain,
    w_out,
    mixer_norm_gain,
    w_up,
    w_down,
):
    tp_size = lax.axis_size("tp")
    seq_group, new_rows, piece_width = tokens.shape
    seq_dev = carried.shape[0]
    gathered = lax.all_gather(tokens, ("kv", "tp"), axis=2, tiled=True)
    normed = norm_rows(gathered, norm_mix)
    model_width = gathered.shape[2]

    def project(weight):
        return jnp.einsum(
            "snd,dhk->snhk", normed, weight, preferred_element_type=jnp.float32
        ).astype(jnp.bfloat16)

    query_raw, forget_raw, value_raw, gate_raw = (
        lax.all_to_all(project(w_query), "kv", split_axis=0, concat_axis=3, tiled=True),
        lax.all_to_all(project(w_forget), "kv", split_axis=0, concat_axis=3, tiled=True),
        lax.all_to_all(project(w_input), "kv", split_axis=0, concat_axis=3, tiled=True),
        lax.all_to_all(project(w_gate), "kv", split_axis=0, concat_axis=3, tiled=True),
    )
    own_lengths = lax.dynamic_slice_in_dim(lengths, lax.axis_index("kv") * seq_dev, seq_dev)
    query_vector = jax.nn.silu(query_raw.astype(jnp.float32))
    forget = lower_bound + (1.0 - lower_bound) * jax.nn.sigmoid(forget_raw.astype(jnp.float32))
    written = 1.0 - forget
    values = value_raw.astype(jnp.float32)
    outer_state = carried
    readouts = []
    for token_position in range(new_rows):
        alive = (token_position < own_lengths)[:, None, None, None]
        updated = (
            forget[:, token_position, :, :, None] * outer_state
            + written[:, token_position, :, :, None] * values[:, token_position, :, None, :]
        )
        outer_state = jnp.where(alive, updated, outer_state)
        state_readout = jnp.einsum(
            "shk,shkv->shv",
            query_vector[:, token_position],
            outer_state,
            precision=lax.Precision.HIGHEST,
        )
        readouts.append(jnp.where(alive[..., 0], state_readout, jnp.float32(0.0)))
    state_readout = jnp.stack(readouts, axis=1)
    scaled = state_readout * lax.rsqrt(
        jnp.mean(state_readout * state_readout, axis=-1, keepdims=True) + 1e-06
    )
    mixed = (scaled * head_gain * jax.nn.silu(gate_raw.astype(jnp.float32))).astype(jnp.bfloat16)
    branch = jnp.einsum(
        "snhv,hvd->snd",
        lax.all_gather(mixed, "kv", axis=0, tiled=True),
        w_out,
        preferred_element_type=jnp.float32,
    )
    pair_width = piece_width * tp_size
    summed_total = lax.psum(branch, "tp")
    pair_cols = lax.dynamic_slice_in_dim(gathered, lax.axis_index("kv") * pair_width, pair_width, 2)
    pair_mid = (pair_cols.astype(jnp.float32) + summed_total).astype(jnp.bfloat16)
    full_pair = lax.all_gather(pair_mid, "kv", axis=2, tiled=True)
    middle = lax.dynamic_slice_in_dim(pair_mid, lax.axis_index("tp") * piece_width, piece_width, 2)
    hidden_in = norm_rows(full_pair, mixer_norm_gain).reshape(seq_group * new_rows, model_width)
    upward = jnp.dot(hidden_in, w_up, preferred_element_type=jnp.float32)
    activated = jnp.square(jax.nn.relu(upward)).astype(jnp.bfloat16)
    collected = lax.psum_scatter(
        jnp.einsum("fd,rf->dr", w_down, activated, preferred_element_type=jnp.float32),
        ("kv", "tp"),
        scatter_dimension=0,
        tiled=True,
    )
    down_part = collected.T.reshape(seq_group, new_rows, piece_width)
    alive_rows = (jnp.arange(new_rows)[None, :] < lengths[:, None])[:, :, None]
    result = jnp.where(alive_rows, middle.astype(jnp.float32) + down_part, jnp.float32(0.0)).astype(
        jnp.bfloat16
    )
    return (result, outer_state)


MESH = pl.DeviceIdType.MESH
F32 = jnp.float32
BF16 = jnp.bfloat16


def step_kernel(
    kv_size,
    tp_size,
    tokens,
    lengths,
    carried,
    norm_mix,
    w_query,
    w_forget,
    w_input,
    w_gate,
    lower_bound,
    head_gain,
    w_out,
    mixer_gain,
    w_up,
    w_down,
    result,
    new_state,
    tok_own,
    tok_all,
    wide,
    state_v,
    state_new,
    norm_v,
    w_proj,
    w_turned,
    lower_v,
    head_v,
    w_out_v,
    mixer_v,
    w_up_v,
    w_down_v,
    raw_split,
    swap_src,
    swap_dst,
    by_slot,
    mix_src,
    mix_dst,
    mix_wide,
    pair_src,
    pair_dst,
    mid_src,
    mid_dst,
    red_src,
    red_dst,
    result_v,
    load_sem,
    send_tok,
    recv_tok,
    send_swap,
    recv_swap,
    send_mix,
    recv_mix,
    send_pair,
    recv_pair,
    send_mid,
    recv_mid,
    send_red,
    recv_red,
    store_sem,
):
    seqs, slots, piece = tok_own.shape
    group = kv_size * tp_size
    rows = seqs * slots
    heads, chans = lower_v.shape
    width = group * piece
    pair = tp_size * piece
    own_cols = w_proj.shape[1]
    sub = own_cols // heads
    per_tile = chans // sub
    kv = lax.axis_index("kv")
    tp = lax.axis_index("tp")
    me = kv * tp_size + tp

    loads = [
        pltpu.make_async_copy(tokens, tok_own, load_sem.at[0]),
        pltpu.make_async_copy(norm_mix, norm_v, load_sem.at[1]),
        pltpu.make_async_copy(w_query, w_proj.at[0], load_sem.at[2]),
        pltpu.make_async_copy(w_forget, w_proj.at[1], load_sem.at[3]),
        pltpu.make_async_copy(w_input, w_proj.at[2], load_sem.at[4]),
        pltpu.make_async_copy(w_gate, w_proj.at[3], load_sem.at[5]),
        pltpu.make_async_copy(lower_bound, lower_v, load_sem.at[6]),
        pltpu.make_async_copy(head_gain, head_v, load_sem.at[7]),
        pltpu.make_async_copy(carried, state_v, load_sem.at[8]),
        pltpu.make_async_copy(w_out, w_out_v, load_sem.at[9]),
        pltpu.make_async_copy(mixer_gain, mixer_v, load_sem.at[10]),
        pltpu.make_async_copy(w_up, w_up_v, load_sem.at[11]),
        pltpu.make_async_copy(w_down, w_down_v, load_sem.at[12]),
    ]
    early = (0, 2, 3, 4, 5, 1, 6, 7)
    for index in early:
        loads[index].start()

    mirrored = [kv, kv + 1 - 2 * lax.rem(kv, 2), lax.rem(kv + 2, 4), 3 - kv]

    def along(step):
        return mirrored[step] if kv_size == 4 else lax.rem(kv + step, kv_size)

    def peer(step):
        hop, side = divmod(step, tp_size)
        column, core = along(hop), lax.rem(tp + side, tp_size)
        return column * tp_size + core, {"kv": column, "tp": core}

    def column_peer(step):
        other = along(step)
        return other, {"kv": other, "tp": tp}

    barrier = pltpu.get_barrier_semaphore()
    for step in range(1, group):
        pl.semaphore_signal(barrier, inc=1, device_id=peer(step)[1], device_id_type=MESH)
    pl.semaphore_wait(barrier, group - 1)

    sent = []

    def send(src, dst, send_sem, recv_sem, device):
        copy = pltpu.make_async_remote_copy(
            src_ref=src,
            dst_ref=dst,
            send_sem=send_sem,
            recv_sem=recv_sem,
            device_id=device,
            device_id_type=MESH,
        )
        copy.start()
        sent.append(copy)

    def arrived(src, dst, send_sem, recv_sem, device):
        pltpu.make_async_remote_copy(
            src_ref=src,
            dst_ref=dst,
            send_sem=send_sem,
            recv_sem=recv_sem,
            device_id=device,
            device_id_type=MESH,
        ).wait_recv()

    def far_first(count):
        return range(count - 1, 0, -1)

    loads[0].wait()
    for step in far_first(group):
        _, device = peer(step)
        send(tok_own, tok_all.at[me], send_tok.at[step], recv_tok.at[me], device)
    tok_all[pl.ds(me, 1)] = tok_own[...][None]
    for index in (1, 6, 7):
        loads[index].wait()
    for matrix in range(4):
        loads[2 + matrix].wait()
        loads[8 + matrix].start()
        w_turned[matrix] = w_proj[matrix].T
    loads[12].start()
    loads[8].wait()
    state_half = state_v[...].reshape(heads * chans, chans).astype(BF16)
    for step in range(1, group):
        other, device = peer(step)
        arrived(tok_own, tok_all.at[other], send_tok.at[step], recv_tok.at[other], device)
    for part in range(group):
        block = tok_all[part].astype(F32)
        for seq in range(seqs):
            wide[seq * slots : (seq + 1) * slots, part * piece : (part + 1) * piece] = block[seq]
    floated = wide[...]
    normed = (
        floated
        * lax.rsqrt(jnp.mean(floated * floated, axis=-1, keepdims=True) + 1e-06)
        * norm_v[...]
    ).astype(BF16)
    for matrix in range(4):
        raw = jnp.dot(normed, w_turned[matrix], preferred_element_type=F32)
        for seq in range(seqs):
            raw_split[seq, matrix * slots : (matrix + 1) * slots, :] = raw[
                seq * slots : (seq + 1) * slots
            ]
    swap_src[...] = raw_split[...].astype(BF16)
    for step in far_first(kv_size):
        other, device = column_peer(step)
        send(swap_src.at[other], swap_dst.at[kv], send_swap.at[step], recv_swap.at[kv], device)
    swap_dst[pl.ds(kv, 1)] = swap_src[pl.ds(kv, 1)]
    for step in range(1, kv_size):
        other, device = column_peer(step)
        arrived(
            swap_src.at[other],
            swap_dst.at[other],
            send_swap.at[step],
            recv_swap.at[other],
            device,
        )

    lane = lax.broadcasted_iota(jnp.int32, (4 * slots, chans), 1) // sub
    arrivals = [swap_dst[part].astype(F32) for part in range(kv_size)]
    for head in range(heads):
        tile, place = divmod(head, per_tile)
        joined = None
        for part in range(kv_size):
            piece_of = arrivals[part][:, tile * chans : (tile + 1) * chans]
            shift = ((part - place) * sub) % chans
            turned = pltpu.roll(piece_of, shift, 1) if shift else piece_of
            joined = turned if joined is None else jnp.where(lane == part, turned, joined)
        by_slot[:, head, :] = joined

    length = lengths[kv]
    lower = lower_v[...]
    queries, forgets, writes, values, gates = [], [], [], [], []
    for slot in range(slots):
        alive = slot < length
        query_raw = by_slot[slot]
        gate_raw = by_slot[3 * slots + slot]
        queries.append(query_raw * jax.nn.sigmoid(query_raw))
        gates.append(gate_raw * jax.nn.sigmoid(gate_raw))
        forget = lower + (1.0 - lower) * jax.nn.sigmoid(by_slot[slots + slot])
        forgets.append(jnp.where(alive, forget, 1.0))
        writes.append(jnp.where(alive, 1.0 - forget, 0.0))
        values.append(by_slot[2 * slots + slot])
    decayed, total = [], None
    for slot in range(slots):
        total = forgets[slot] if total is None else total * forgets[slot]
        decayed.append(queries[slot] * total)
    stacked = jnp.concatenate(decayed, axis=0)
    row_head = lax.broadcasted_iota(jnp.int32, (slots * heads, chans), 0) % heads
    spread = jnp.concatenate(
        [jnp.where(row_head == head, stacked, 0.0).astype(BF16) for head in range(heads)], axis=1
    )
    from_state = jnp.dot(spread, state_half, preferred_element_type=F32)
    kept = list(writes)
    for slot in range(slots):
        for earlier in range(slot):
            kept[earlier] = kept[earlier] * forgets[slot]
        readout = from_state[slot * heads : (slot + 1) * heads]
        for earlier in range(slot + 1):
            weight = jnp.sum(queries[slot] * kept[earlier], axis=-1, keepdims=True)
            readout = readout + weight * values[earlier]
        readout = jnp.where(slot < length, readout, 0.0)
        scaled = readout * lax.rsqrt(jnp.mean(readout * readout, axis=-1, keepdims=True) + 1e-06)
        mix_src[slot] = (scaled * head_v[...] * gates[slot]).astype(BF16)
    for step in far_first(kv_size):
        other, device = column_peer(step)
        send(mix_src, mix_dst.at[kv], send_mix.at[step], recv_mix.at[kv], device)
    mix_dst[pl.ds(kv, 1)] = mix_src[...][None]

    columns = jnp.concatenate([total] + kept, axis=0).T
    for head in range(heads):
        fresh = columns[:, head : head + 1] * state_v[head]
        for slot in range(slots):
            at = (slot + 1) * heads + head
            fresh = fresh + columns[:, at : at + 1] * values[slot][head : head + 1]
        state_new[head] = fresh
    state_store = pltpu.make_async_copy(state_new, new_state, store_sem.at[0])
    state_store.start()

    for step in range(1, kv_size):
        other, device = column_peer(step)
        arrived(mix_src, mix_dst.at[other], send_mix.at[step], recv_mix.at[other], device)
    mix_wide[...] = mix_dst[...].astype(F32).reshape(rows, heads, chans)
    mixed = jnp.concatenate([mix_wide[:, head, :].astype(BF16) for head in range(heads)], axis=1)
    loads[9].wait()
    partial = jnp.dot(mixed, w_out_v[...], preferred_element_type=F32)
    pair_src[...] = partial
    partner = {"kv": kv, "tp": lax.rem(tp + 1, tp_size)}
    send(pair_src, pair_dst, send_pair.at[0], recv_pair.at[0], partner)
    own_wide = wide[:, pl.ds(pl.multiple_of(kv * pair, pair), pair)]
    arrived(pair_src, pair_dst, send_pair.at[0], recv_pair.at[0], partner)
    mid_src[...] = (own_wide + (partial + pair_dst[...])).astype(BF16)
    for step in far_first(kv_size):
        other, device = column_peer(step)
        send(mid_src, mid_dst.at[kv], send_mid.at[step], recv_mid.at[kv], device)
    mid_dst[pl.ds(kv, 1)] = mid_src[...][None]
    for step in range(1, kv_size):
        other, device = column_peer(step)
        arrived(mid_src, mid_dst.at[other], send_mid.at[step], recv_mid.at[other], device)

    middle = jnp.concatenate([mid_dst[part].astype(F32) for part in range(kv_size)], axis=1)
    loads[10].wait()
    hidden = (
        middle
        * lax.rsqrt(jnp.mean(middle * middle, axis=-1, keepdims=True) + 1e-06)
        * mixer_v[...]
    ).astype(BF16)
    loads[11].wait()
    upward = jnp.dot(hidden, w_up_v[...], preferred_element_type=F32)
    activated = jnp.square(jnp.maximum(upward, 0.0)).astype(BF16)
    loads[12].wait()

    def down_piece(other):
        cols = pl.ds(pl.multiple_of(other * piece, piece), piece)
        return jnp.dot(activated, w_down_v[:, cols], preferred_element_type=F32)

    for step in far_first(group):
        other, device = peer(step)
        red_src[step] = down_piece(other).astype(BF16)
        send(red_src.at[step], red_dst.at[me], send_red.at[step], recv_red.at[me], device)
    down = down_piece(me)
    own_mid = mid_src[:, pl.ds(pl.multiple_of(tp * piece, piece), piece)].astype(F32)
    for step in range(1, group):
        other, device = peer(step)
        arrived(red_src.at[step], red_dst.at[other], send_red.at[step], recv_red.at[other], device)
        down = down + red_dst[other].astype(F32)
    done = own_mid + down
    slot_of = lax.broadcasted_iota(jnp.int32, (slots, piece), 0)
    for seq in range(seqs):
        kept_rows = jnp.where(
            slot_of < lengths[seq], done[seq * slots : (seq + 1) * slots], 0.0
        )
        result_v[seq] = kept_rows.astype(BF16)
    result_store = pltpu.make_async_copy(result_v, result, store_sem.at[1])
    result_store.start()
    for copy in sent:
        copy.wait_send()
    state_store.wait()
    result_store.wait()


def store_kernel(result, new_state, result_out, state_out, small, large, load_sem, store_sem):
    heads = large.shape[0]
    parts = 4 if heads % 4 == 0 else 1
    chunk = heads // parts
    hops = [(result, small, result_out)]
    for part in range(parts):
        own = pl.ds(part * chunk, chunk)
        hops.append((new_state.at[own], large.at[own], state_out.at[own]))
    inward = [
        pltpu.make_async_copy(src, held, load_sem.at[at])
        for at, (src, held, _) in enumerate(hops)
    ]
    outward = [
        pltpu.make_async_copy(held, dst, store_sem.at[at])
        for at, (_, held, dst) in enumerate(hops)
    ]
    for copy in inward:
        copy.start()
    for before, after in zip(inward, outward):
        before.wait()
        after.start()
    for copy in outward:
        copy.wait()


def local_kernel(
    tokens,
    lengths,
    carried,
    norm_mix,
    w_query,
    w_forget,
    w_input,
    w_gate,
    lower_bound,
    head_gain,
    w_out,
    mixer_norm_gain,
    w_up,
    w_down,
):
    kv_size = lax.axis_size("kv")
    tp_size = lax.axis_size("tp")
    group = kv_size * tp_size
    seqs, slots, piece = tokens.shape
    _, heads, chans, _ = carried.shape
    model, _, sub = w_query.shape
    rows, pair, cols = seqs * slots, piece * tp_size, heads * sub
    hidden = w_up.shape[1]

    def turned(weight):
        return weight.transpose(1, 2, 0).reshape(cols, model)

    anywhere = pl.BlockSpec(memory_space=pl.ANY)
    dma = pltpu.SemaphoreType.DMA
    vmem = pltpu.VMEM
    result, new_state = pl.pallas_call(
        functools.partial(step_kernel, kv_size, tp_size),
        out_shape=(
            jax.ShapeDtypeStruct(tokens.shape, BF16),
            jax.ShapeDtypeStruct((heads, chans, chans), F32),
        ),
        in_specs=[anywhere, pl.BlockSpec(memory_space=pltpu.SMEM)] + [anywhere] * 12,
        out_specs=(anywhere, anywhere),
        scratch_shapes=[
            vmem((seqs, slots, piece), BF16),
            vmem((group, seqs, slots, piece), BF16),
            vmem((rows, model), F32),
            vmem((heads, chans, chans), F32),
            vmem((heads, chans, chans), F32),
            vmem((1, model), F32),
            vmem((4, cols, model), BF16),
            vmem((4, model, cols), BF16),
            vmem((heads, chans), F32),
            vmem((1, chans), F32),
            vmem((heads * chans, pair), BF16),
            vmem((1, model), F32),
            vmem((model, hidden), BF16),
            vmem((hidden, model), BF16),
            vmem((seqs, 4 * slots, cols), F32),
            vmem((seqs, 4 * slots, cols), BF16),
            vmem((kv_size, 4 * slots, cols), BF16),
            vmem((4 * slots, heads, chans), F32),
            vmem((slots, heads, chans), BF16),
            vmem((kv_size, slots, heads, chans), BF16),
            vmem((rows, heads, chans), F32),
            vmem((rows, pair), F32),
            vmem((rows, pair), F32),
            vmem((rows, pair), BF16),
            vmem((kv_size, rows, pair), BF16),
            vmem((group, rows, piece), BF16),
            vmem((group, rows, piece), BF16),
            vmem((seqs, slots, piece), BF16),
            dma((13,)),
            dma((group,)),
            dma((group,)),
            dma((kv_size,)),
            dma((kv_size,)),
            dma((kv_size,)),
            dma((kv_size,)),
            dma((1,)),
            dma((1,)),
            dma((kv_size,)),
            dma((kv_size,)),
            dma((group,)),
            dma((group,)),
            dma((2,)),
        ],
        compiler_params=pltpu.CompilerParams(
            collective_id=0, has_side_effects=True, vmem_limit_bytes=60000 * 1024
        ),
    )(
        tokens,
        lengths,
        carried.reshape(heads, chans, chans),
        norm_mix.reshape(1, model),
        turned(w_query),
        turned(w_forget),
        turned(w_input),
        turned(w_gate),
        lower_bound,
        head_gain.reshape(1, chans),
        w_out.reshape(heads * chans, pair),
        mixer_norm_gain.reshape(1, model),
        w_up,
        w_down,
    )
    result, new_state = pl.pallas_call(
        store_kernel,
        out_shape=(
            jax.ShapeDtypeStruct(tokens.shape, BF16),
            jax.ShapeDtypeStruct((heads, chans, chans), F32),
        ),
        in_specs=[anywhere] * 2,
        out_specs=(anywhere, anywhere),
        scratch_shapes=[
            vmem(tokens.shape, BF16),
            vmem((heads, chans, chans), F32),
            dma((5,)),
            dma((5,)),
        ],
        compiler_params=pltpu.CompilerParams(vmem_limit_bytes=60000 * 1024),
    )(result, new_state)
    return result, new_state.reshape(carried.shape)


def local(*arrays):
    tokens, carried, weight = arrays[0], arrays[2], arrays[4]
    aligned = (
        tokens.shape[2] % 128 == 0
        and carried.shape[0] == 1
        and carried.shape[2] % 128 == 0
        and carried.shape[2] % weight.shape[2] == 0
        and (weight.shape[1] * weight.shape[2]) % carried.shape[2] == 0
        and lax.axis_size("tp") == 2
        and tokens.shape[1] % 4 == 0
    )
    return (local_kernel if aligned else local_collectives)(*arrays)


def solution(mesh):
    placed = (
        P("dp", None, ("kv", "tp")),
        P("dp"),
        P(("dp", "kv"), "tp", None, None),
        P(),
        P(None, "tp", "kv"),
        P(None, "tp", "kv"),
        P(None, "tp", "kv"),
        P(None, "tp", "kv"),
        P("tp", None),
        P(),
        P("tp", None, "kv"),
        P(),
        P(None, ("kv", "tp")),
        P(("kv", "tp"), None),
    )
    return jax.shard_map(
        local,
        mesh=mesh,
        in_specs=placed,
        out_specs=(P("dp", None, ("kv", "tp")), P(("dp", "kv"), "tp", None, None)),
        check_vma=False,
    )
```
